32 devices in a mesh: grp: 2 (over y), sp: 4 (over z), tp: 4 (over x, core).
Axes of the slice: x: 2, y: 2, z: 4, core: 2. Of those that a mesh axis runs over, the one named last changes fastest.
Arguments:
- window_query: bfloat16 [2560, 2048], P(('grp', 'sp'), 'tp'), parts along dimension 0, may hold values from -24 to 24
- window_key: bfloat16 [2560, 1024], P(('grp', 'sp'), 'tp'), parts along dimension 0, may hold values from -24 to 24
- window_value: bfloat16 [2560, 1024], P(('grp', 'sp'), 'tp'), parts along dimension 0, may hold values from -6 to 6
- grid_query: bfloat16 [2560, 2048], P(('grp', 'sp'), 'tp'), parts along dimension 0, may hold values from -10 to 10
- grid_key: bfloat16 [2560, 1024], P(('grp', 'sp'), 'tp'), parts along dimension 0, may hold values from -10 to 10
- grid_value: bfloat16 [2560, 1024], P(('grp', 'sp'), 'tp'), parts along dimension 0, may hold values from -6 to 6
- sink_logit: float32 [16], P('tp'), may hold values from 1 to 6
- query_gain: float32 [128], replicated, may hold values from 0.8 to 6
- key_gain: float32 [128], replicated, may hold values from 0.8 to 6
- window_weights: bfloat16 [2048, 4096], P('tp'), may hold values from -0.59765625 to 0.59765625
- grid_weights: bfloat16 [2048, 4096], P('tp'), may hold values from -0.59765625 to 0.59765625
Outputs:
- merged: bfloat16 [2560, 4096], P(('grp', 'sp', 'tp')), parts along dimension 0
The draws below stay inside these ranges and needn't reach their ends.
There are 2 independent parts, one for each index of `grp`. The reference program is written for one: setup_inputs(seed, part) draws one part's arguments, and reference() takes and returns one part's arrays. A program takes and returns all parts, laid end to end along the dimension named above; an argument that names none is the same for every part. Nothing has to cross between parts.
All inputs are finite; a program needn't handle non-finite values.
Results may differ from the reference program's by a relative error of at most 0.014.
The reference program's roundings to bfloat16 on the way count: a program that leaves them out, or rounds other values in their place, can miss the bound.
Values may be sent and summed in bfloat16 or wider, within the bound.
A program may use at most 64 MiB of HBM per device.

```python
import jax
import jax.numpy as jnp
from jax import lax

D = 4096
HEAD = 128
QH_A = 16
KVH_A = 8
QH_B = 16
KVH_B = 8
WINDOW = 128
GRID_W = 64
TOKENS = 1280
N_SP = 4
N_TP = 4


def pair_window(key):
    base = jax.random.fold_in(key, 101)
    key_query, key_key = jax.random.split(base, 2)
    queries = jnp.clip(jax.random.normal(key_query, (TOKENS, QH_A * HEAD), jnp.float32), -6.0, 6.0)
    keys = jnp.clip(jax.random.normal(key_key, (TOKENS, KVH_A * HEAD), jnp.float32), -6.0, 6.0)
    return (queries, keys)


def pair_grid(key):
    base = jax.random.fold_in(key, 202)
    key_query, key_key = jax.random.split(base, 2)
    queries = jnp.clip(jax.random.normal(key_query, (TOKENS, QH_B * HEAD), jnp.float32), -6.0, 6.0)
    keys = jnp.clip(jax.random.normal(key_key, (TOKENS, KVH_B * HEAD), jnp.float32), -6.0, 6.0)
    return (queries, keys)


def grid_gain(key, salt):
    base = jax.random.fold_in(key, salt)
    return 1.5 + 0.27 * jnp.clip(jax.random.normal(base, (HEAD,), jnp.float32), -2.5, 2.5)


def draw_window_query(key, part):
    return pair_window(key)[0].astype(jnp.bfloat16)


def draw_window_key(key, part):
    return pair_window(key)[1].astype(jnp.bfloat16)


def draw_grid_query(key, part):
    return pair_grid(key)[0].astype(jnp.bfloat16)


def draw_grid_key(key, part):
    return pair_grid(key)[1].astype(jnp.bfloat16)


def draw_query_gain(key, part):
    return grid_gain(key, 303)


def draw_key_gain(key, part):
    return grid_gain(key, 404)


def steps_of(rng, dims, shards, low, high):
    def one(dim, blocks):
        heights = jax.random.uniform(jax.random.fold_in(jax.random.fold_in(rng, 6), dim), (blocks,), jnp.float32, low / len(shards), high / len(shards))
        return jnp.repeat(jnp.exp(heights), dims[dim] // blocks).reshape((-1,) + (1,) * (len(dims) - dim - 1))

    loudness = one(*shards[0])
    for cut in shards[1:]:
        loudness = loudness * one(*cut)
    return loudness


def noise(own_key, extent, scale, most, cuts=(), held_as=jnp.bfloat16):
    entries = scale * jax.random.normal(own_key, extent, jnp.float32)
    if cuts:
        entries = entries * steps_of(own_key, extent, cuts, -0.22, 0.18)
    return jnp.clip(entries, -most, most).astype(held_as)


def setup_inputs(seed: int = 0, part: int = 0) -> dict:
    key_list = jax.random.split(jax.random.key(seed), 12)
    part_keys = jax.random.split(jax.random.fold_in(key_list[11], part), 12)
    return {
        "window_query": draw_window_query(jax.random.fold_in(jax.random.fold_in(key_list[11], part), 71), part),
        "window_key": draw_window_key(jax.random.fold_in(jax.random.fold_in(key_list[11], part), 71), part),
        "window_value": noise(part_keys[2], (TOKENS, KVH_A * HEAD), 1.0, 6.0, ((0, 4), (1, 4))),
        "grid_query": draw_grid_query(jax.random.fold_in(jax.random.fold_in(key_list[11], part), 71), part),
        "grid_key": draw_grid_key(jax.random.fold_in(jax.random.fold_in(key_list[11], part), 71), part),
        "grid_value": noise(part_keys[5], (TOKENS, KVH_B * HEAD), 1.0, 6.0, ((0, 4), (1, 4))),
        "sink_logit": jnp.clip(1.0 + 5.0 * jax.random.uniform(key_list[6], (QH_A,), jnp.float32) ** steps_of(key_list[6], (QH_A,), ((0, 4),), -0.2, 0.2), 1.0, 6.0),
        "query_gain": draw_query_gain(jax.random.fold_in(key_list[11], 71), part),
        "key_gain": draw_key_gain(jax.random.fold_in(key_list[11], 71), part),
        "window_weights": noise(key_list[9], (QH_A * HEAD, D), 0.1, 0.59765625, ((0, 4),)),
        "grid_weights": noise(key_list[10], (QH_B * HEAD, D), 0.1, 0.59765625, ((0, 4),)),
    }


THETA = 10000.0
NEGATIVE = -1e+30
EPSILON = 1e-06

def turn_section(values, places):
    width = values.shape[-1]
    half_width = width // 2
    frequency = THETA ** (-jnp.arange(0, width, 2, dtype=jnp.float32) / width)
    angles = places[:, None] * frequency[None, :]
    cosine = jnp.cos(angles)[:, None, :]
    sine_part = jnp.sin(angles)[:, None, :]
    first_half = values[..., :half_width]
    second_half = values[..., half_width:]
    return jnp.concatenate([first_half * cosine - second_half * sine_part, second_half * cosine + first_half * sine_part], axis=-1)

def normed_turn(values, gain, places):
    count_rows = values.shape[0]
    shaped = values.astype(jnp.float32).reshape(count_rows, -1, HEAD)
    scaled = shaped * lax.rsqrt(lax.optimization_barrier(jnp.mean(shaped * shaped, axis=-1, keepdims=True)) + EPSILON)
    scaled = scaled * gain.astype(jnp.float32)
    grid_row = (places // GRID_W).astype(jnp.float32)
    grid_col = (places % GRID_W).astype(jnp.float32)
    section = HEAD // 2
    turned = jnp.concatenate([turn_section(scaled[..., :section], grid_row), turn_section(scaled[..., section:], grid_col)], axis=-1)
    return turned.astype(jnp.bfloat16)

def window_attend(queries, keys_pad, values_pad, slopes, sink_logits, offset, total_rows):
    query_rows = queries.shape[0]
    block_span = WINDOW // 2
    blocks = query_rows // block_span
    key_heads = keys_pad.shape[1] // HEAD
    group_size = queries.shape[1] // keys_pad.shape[1]
    query_blocks = queries.astype(jnp.float32).reshape(blocks, block_span, key_heads, group_size, HEAD)
    key_blocks = keys_pad.astype(jnp.float32).reshape(blocks + 4, block_span, key_heads, HEAD)
    value_blocks = values_pad.astype(jnp.float32).reshape(blocks + 4, block_span, key_heads, HEAD)
    key_window = jnp.concatenate([key_blocks[block_shift:block_shift + blocks] for block_shift in range(5)], axis=1)
    value_window = jnp.concatenate([value_blocks[block_shift:block_shift + blocks] for block_shift in range(5)], axis=1)
    scores = jnp.einsum('nqkgd,nskd->kgnqs', query_blocks, key_window) * HEAD ** (-0.5)
    query_place = offset + jnp.arange(query_rows, dtype=jnp.int32).reshape(blocks, block_span, 1)
    key_place = offset - WINDOW + block_span * jnp.arange(blocks, dtype=jnp.int32)[:, None, None] + jnp.arange(5 * block_span, dtype=jnp.int32)[None, None, :]
    distance = jnp.abs(key_place - query_place)
    inside = (distance <= WINDOW) & (key_place >= 0) & (key_place < total_rows)
    slope_grid = slopes.reshape(key_heads, group_size, 1, 1, 1)
    sink_grid = sink_logits.astype(jnp.float32).reshape(key_heads, group_size, 1, 1)
    scores = jnp.where(inside, scores - slope_grid * distance.astype(jnp.float32), NEGATIVE)
    highest = jnp.maximum(lax.optimization_barrier(jnp.max(scores, axis=-1)), sink_grid)
    raised = jnp.exp(scores - highest[..., None])
    denominator = lax.optimization_barrier(jnp.sum(raised, axis=-1)) + jnp.exp(sink_grid - highest)
    weights = lax.optimization_barrier((raised / denominator[..., None]).astype(jnp.bfloat16))
    attended = jnp.einsum('kgnqs,nskd->nqkgd', weights.astype(jnp.float32), value_window)
    return attended.astype(jnp.bfloat16).reshape(query_rows, -1)

def reference(window_query, window_key, window_value, grid_query, grid_key, grid_value, sink_logit, query_gain, key_gain, window_weights, grid_weights):
    total_rows = window_query.shape[0]
    places = jnp.arange(total_rows, dtype=jnp.int32)
    slopes = 2.0 ** (-8.0 * jnp.arange(1, QH_A + 1, dtype=jnp.float32) / QH_A)
    padding = ((WINDOW, WINDOW), (0, 0))
    window_out = window_attend(window_query, jnp.pad(window_key, padding), jnp.pad(window_value, padding), slopes, sink_logit, 0, total_rows)
    group_size = QH_B // KVH_B
    turned_q = lax.optimization_barrier(normed_turn(grid_query, query_gain, places))
    turned_q = turned_q.astype(jnp.float32).reshape(total_rows, KVH_B, group_size, HEAD)
    turned_k = lax.optimization_barrier(normed_turn(grid_key, key_gain, places))
    key_pieces = turned_k.astype(jnp.float32).reshape(N_SP, total_rows // N_SP, KVH_B, HEAD)
    value_pieces = grid_value.astype(jnp.float32).reshape(N_SP, total_rows // N_SP, KVH_B, HEAD)

    def absorb(carry, block_pair):
        highest, summed, gathered = carry
        key_block, value_block = block_pair
        scores = jnp.einsum('tkgd,skd->kgts', turned_q, key_block) * HEAD ** (-0.5)
        raised_top = jnp.maximum(highest, lax.optimization_barrier(jnp.max(scores, axis=-1)))
        fading = jnp.exp(highest - raised_top)
        raised = jnp.exp(scores - raised_top[..., None])
        summed = summed * fading + lax.optimization_barrier(jnp.sum(raised, axis=-1))
        rounded = lax.optimization_barrier(raised.astype(jnp.bfloat16)).astype(jnp.float32)
        gathered = gathered * fading[..., None] + jnp.einsum('kgts,skd->kgtd', rounded, value_block)
        return ((raised_top, summed, gathered), None)
    start_carry = (jnp.full((KVH_B, group_size, total_rows), NEGATIVE, jnp.float32), jnp.zeros((KVH_B, group_size, total_rows), jnp.float32), jnp.zeros((KVH_B, group_size, total_rows, HEAD), jnp.float32))
    final_carry, _ = lax.scan(absorb, start_carry, (key_pieces, value_pieces))
    grid_out = (final_carry[2] / final_carry[1][..., None]).astype(jnp.bfloat16)
    width_a = QH_A // N_TP * HEAD
    heads_b = KVH_B // N_TP
    shaped_b = grid_weights.reshape(KVH_B, group_size, HEAD, D)

    def group_term(running, group_index):
        part_a = lax.dynamic_slice_in_dim(window_out, group_index * width_a, width_a, 1)
        rows_a = lax.dynamic_slice_in_dim(window_weights, group_index * width_a, width_a, 0)
        part_b = lax.dynamic_slice_in_dim(grid_out, group_index * heads_b, heads_b, 0)
        rows_b = lax.dynamic_slice_in_dim(shaped_b, group_index * heads_b, heads_b, 0)
        partial_term = jnp.dot(part_a, rows_a, preferred_element_type=jnp.float32)
        partial_term = partial_term + jnp.einsum('kgtd,kgdo->to', part_b.astype(jnp.float32), rows_b.astype(jnp.float32))
        partial_term = lax.optimization_barrier(partial_term.astype(jnp.bfloat16)).astype(jnp.float32)
        return (running + partial_term, None)
    merged, _ = lax.scan(group_term, jnp.zeros((total_rows, D), jnp.float32), jnp.arange(N_TP, dtype=jnp.int32))
    return merged.astype(jnp.bfloat16)
```

```python
import functools
import math

import jax
import jax.numpy as jnp
from jax import lax
from jax.experimental import pallas as pl
from jax.experimental.pallas import tpu as pltpu
from jax.sharding import PartitionSpec as P

HEAD = 128
QH_A = 16
WINDOW = 128
GRID_W = 64
THETA = 10000.0
NEGATIVE = -1e30
EPSILON = 1e-06
MESH = pl.DeviceIdType.MESH
F32 = jnp.float32
BF16 = jnp.bfloat16


def dot_nt(a, b):
    return lax.dot_general(a, b, (((1,), (1,)), ((), ())), preferred_element_type=F32)


def dot_tn(a, b):
    return lax.dot_general(a, b, (((0,), (0,)), ((), ())), preferred_element_type=F32)


def kernel(
    n, n_tp, rows, kvh, group, chunks,
    wq_hbm, wk_hbm, wv_hbm, gq_hbm, gk_hbm, gv_hbm, sink_ref, qgain_ref, kgain_ref, ww_hbm, gw_hbm,
    out_ref,
    qw, wkv, qraw, kraw, qg, kvbuf, ww, gw, cosine, sine, top, total, acc, attn, proj, pbuf, dbuf, sbuf, rbuf, own,
    lsem, gsend, grecv, hsend, hrecv, dsend, drecv, xsend, xrecv,
):
    me = lax.axis_index("sp")
    t = lax.axis_index("tp")
    core = lax.rem(t, 2)
    x = t // 2
    n_x = n_tp // 2
    partner = x * 2 + 1 - core
    out_rows = rows // n_tp
    width = ww.shape[1] // chunks
    span = group * rows
    has_left = me > 0
    has_right = me < n - 1

    loads = []

    def load(src, dst):
        copy = pltpu.make_async_copy(src, dst, lsem.at[len(loads)])
        copy.start()
        loads.append(copy)
        return copy

    def head_cols(h):
        return slice(h * HEAD, (h + 1) * HEAD)

    k_loads = [load(gk_hbm.at[:, head_cols(g)], kraw.at[g]) for g in range(kvh)]
    v_loads = [load(gv_hbm.at[:, head_cols(g)], kvbuf.at[me, g, 1]) for g in range(kvh)]
    w_loads = []
    for g in range(kvh):
        w_loads.append(load(wk_hbm.at[:, head_cols(g)], wkv.at[g, 0, WINDOW : WINDOW + rows]))
        w_loads.append(load(wv_hbm.at[:, head_cols(g)], wkv.at[g, 1, WINDOW : WINDOW + rows]))
    q_loads = []
    for g in range(kvh):
        for u in range(group):
            q_loads.append(load(gq_hbm.at[:, head_cols(g * group + u)], qraw.at[g, u * rows : (u + 1) * rows]))
    wq_loads = []
    for g in range(kvh):
        for u in range(group):
            wq_loads.append(load(wq_hbm.at[:, head_cols(g * group + u)], qw.at[g, u * rows : (u + 1) * rows]))
    ww_load = load(ww_hbm, ww)
    gw_load = load(gw_hbm, gw)

    barrier = pltpu.get_barrier_semaphore()

    def greet(device):
        pl.semaphore_signal(barrier, inc=1, device_id=device, device_id_type=MESH)

    @pl.when(has_left)
    def _():
        greet({"sp": me - 1})

    @pl.when(has_right)
    def _():
        greet({"sp": me + 1})

    greet({"tp": partner})
    for dx in range(1, n_x):
        greet({"tp": lax.rem(x + dx, n_x) * 2 + core})

    place = me * rows + lax.broadcasted_iota(jnp.int32, (rows, HEAD), 0)
    lane = lax.broadcasted_iota(jnp.int32, (rows, HEAD), 1)
    section = HEAD // 2
    half = section // 2
    frequency = jnp.exp(jnp.bitwise_and(lane, half - 1).astype(F32) * (-2.0 * math.log(THETA) / section))
    position = jnp.where(lane < section, place // GRID_W, lax.rem(place, GRID_W)).astype(F32)
    angle = position * frequency
    low = jnp.bitwise_and(lane, section - 1) < half
    cosine[...] = jnp.cos(angle)
    sine[...] = jnp.where(low, -jnp.sin(angle), jnp.sin(angle))

    def turn(values, gain):
        v = values.astype(F32)
        v = v * lax.rsqrt(jnp.mean(v * v, axis=1, keepdims=True) + EPSILON) * gain
        first = lax.broadcasted_iota(jnp.int32, v.shape, 1)
        other = jnp.where(
            jnp.bitwise_and(first, section - 1) < half,
            pltpu.roll(v, HEAD - half, 1),
            pltpu.roll(v, half, 1),
        )
        return (v * cosine[...] + other * sine[...]).astype(BF16)

    for g in range(kvh):
        k_loads[g].wait()
        kvbuf[me, g, 0] = turn(kraw[g], kgain_ref[...])
    for copy in v_loads:
        copy.wait()

    pl.semaphore_wait(barrier, has_left.astype(jnp.int32) + has_right.astype(jnp.int32) + n_x)

    def block_copy(source, g, direction):
        return pltpu.make_async_remote_copy(
            src_ref=kvbuf.at[source, g],
            dst_ref=kvbuf.at[source, g],
            send_sem=gsend.at[direction, source, g],
            recv_sem=grecv.at[source, g],
            device_id={"sp": me + 1 if direction == 0 else me - 1},
            device_id_type=MESH,
        )

    def halo_copy(direction):
        source = rows if direction == 0 else WINDOW
        target = 0 if direction == 0 else WINDOW + rows
        return pltpu.make_async_remote_copy(
            src_ref=wkv.at[:, :, source : source + WINDOW],
            dst_ref=wkv.at[:, :, target : target + WINDOW],
            send_sem=hsend.at[direction],
            recv_sem=hrecv.at[direction],
            device_id={"sp": me + 1 if direction == 0 else me - 1},
            device_id_type=MESH,
        )

    for g in range(kvh):
        @pl.when(has_right)
        def _():
            block_copy(me, g, 0).start()

        @pl.when(has_left)
        def _():
            block_copy(me, g, 1).start()

    for copy in w_loads:
        copy.wait()

    @pl.when(has_right)
    def _():
        halo_copy(0).start()

    @pl.when(has_left)
    def _():
        halo_copy(1).start()

    @pl.when(jnp.logical_not(has_left))
    def _():
        wkv[:, :, 0:WINDOW] = jnp.zeros((kvh, 2, WINDOW, HEAD), BF16)

    @pl.when(jnp.logical_not(has_right))
    def _():
        wkv[:, :, WINDOW + rows :] = jnp.zeros((kvh, 2, WINDOW, HEAD), BF16)

    for copy in q_loads:
        copy.wait()
    for g in range(kvh):
        for u in range(group):
            part = slice(u * rows, (u + 1) * rows)
            qg[g, part] = turn(qraw[g, part], qgain_ref[...])

    scale = HEAD ** (-0.5)

    def absorb(source, g, first=False):
        scores = dot_nt(kvbuf[source, g, 0], qg[g]) * scale
        block_top = jnp.max(scores, axis=0, keepdims=True)
        if first:
            raised = jnp.exp(scores - block_top)
            top[g] = block_top
            total[g] = jnp.sum(raised, axis=0, keepdims=True)
            acc[g] = dot_tn(kvbuf[source, g, 1], raised.astype(BF16))
        else:
            before = top[g]
            new_top = jnp.maximum(before, block_top)
            fading = jnp.exp(before - new_top)
            raised = jnp.exp(scores - new_top)
            top[g] = new_top
            total[g] = total[g] * fading + jnp.sum(raised, axis=0, keepdims=True)
            acc[g] = acc[g] * fading + dot_tn(kvbuf[source, g, 1], raised.astype(BF16))

    for g in range(kvh):
        absorb(me, g, True)

    def relay(d):
        for g in range(kvh):
            @pl.when(me - d >= 0)
            def _():
                block_copy(me - d, g, 0).wait_recv()

                @pl.when(has_right)
                def _():
                    block_copy(me - d, g, 0).start()

            @pl.when(me + d < n)
            def _():
                block_copy(me + d, g, 1).wait_recv()

                @pl.when(has_left)
                def _():
                    block_copy(me + d, g, 1).start()

            @pl.when(me - d >= 0)
            def _():
                absorb(me - d, g)

            @pl.when(me + d < n)
            def _():
                absorb(me + d, g)

    def put_heads(base, g, value):
        turned = jnp.transpose(value).astype(BF16)
        for u in range(group):
            attn[:, base + (g * group + u) * HEAD : base + (g * group + u + 1) * HEAD] = turned[u * rows : (u + 1) * rows]

    heads_width = kvh * group * HEAD

    def windowed():
        for copy in wq_loads:
            copy.wait()

        @pl.when(has_left)
        def _():
            halo_copy(0).wait_recv()

        @pl.when(has_right)
        def _():
            halo_copy(1).wait_recv()

        padded = rows + 2 * WINDOW
        key_at = lax.broadcasted_iota(jnp.int32, (padded, span), 0) - WINDOW
        column = lax.broadcasted_iota(jnp.int32, (padded, span), 1)
        distance = jnp.abs(key_at - lax.rem(column, rows))
        key_place = me * rows + key_at
        inside = (distance <= WINDOW) & (key_place >= 0) & (key_place < n * rows)
        far = distance.astype(F32)
        member = lax.broadcasted_iota(jnp.int32, (1, span), 1) // rows
        for g in range(kvh):
            head = (t * (kvh * group) + g * group + 1 + member).astype(F32)
            slope = jnp.exp2(head * (-8.0 / QH_A))
            sink = jnp.zeros((1, span), F32)
            for u in range(group):
                sink = jnp.where(member == u, sink_ref[g * group + u], sink)
            scores = dot_nt(wkv[g, 0], qw[g]) * scale
            scores = jnp.where(inside, scores - slope * far, NEGATIVE)
            highest = jnp.maximum(jnp.max(scores, axis=0, keepdims=True), sink)
            raised = jnp.exp(scores - highest)
            bottom = jnp.sum(raised, axis=0, keepdims=True) + jnp.exp(sink - highest)
            weights = (raised * (1.0 / bottom)).astype(BF16)
            put_heads(0, g, dot_tn(wkv[g, 1], weights))
        ww_load.wait()
        for j in range(chunks):
            cols = slice(j * width, (j + 1) * width)
            proj[:, cols] = jnp.dot(attn[:, :heads_width], ww[:, cols], preferred_element_type=F32)

    if n > 1:
        relay(1)
    windowed()
    if n <= 4:
        for d in range(2, n):
            relay(d)
    else:
        def relay_step(d, carry):
            relay(d)
            return carry

        lax.fori_loop(2, n, relay_step, 0)

    for g in range(kvh):
        put_heads(heads_width, g, acc[g] * (1.0 / total[g]))
    gw_load.wait()

    def pair_copy(j):
        return pltpu.make_async_remote_copy(
            src_ref=pbuf.at[j, 1 - core],
            dst_ref=dbuf.at[j],
            send_sem=dsend.at[j],
            recv_sem=drecv.at[j],
            device_id={"tp": partner},
            device_id_type=MESH,
        )

    def cross_copy(j, dx):
        return pltpu.make_async_remote_copy(
            src_ref=sbuf.at[j, dx - 1],
            dst_ref=rbuf.at[j, dx - 1],
            send_sem=xsend.at[j, dx - 1],
            recv_sem=xrecv.at[j, dx - 1],
            device_id={"tp": lax.rem(x + dx, n_x) * 2 + core},
            device_id_type=MESH,
        )

    def pass_on(j):
        pair_copy(j).wait_recv()
        for dx in range(1, n_x):
            other = lax.rem(x + dx, n_x)
            sbuf[j, dx - 1] = (pbuf[j, core, other].astype(F32) + dbuf[j, other].astype(F32)).astype(BF16)
            cross_copy(j, dx).start()
        own[j] = pbuf[j, core, x].astype(F32) + dbuf[j, x].astype(F32)

    for j in range(chunks):
        cols = slice(j * width, (j + 1) * width)
        part = proj[:, cols] + jnp.dot(attn[:, heads_width:], gw[:, cols], preferred_element_type=F32)
        for b in range(n_tp):
            pbuf[j, b % 2, b // 2] = part[b * out_rows : (b + 1) * out_rows].astype(BF16)
        pair_copy(j).start()
        if j >= 1:
            pass_on(j - 1)
    pass_on(chunks - 1)
    for j in range(chunks):
        value = own[j]
        for dx in range(1, n_x):
            cross_copy(j, dx).wait_recv()
            value = value + rbuf[j, dx - 1].astype(F32)
        out_ref[:, j * width : (j + 1) * width] = value.astype(BF16)

    for j in range(chunks):
        pair_copy(j).wait_send()
        for dx in range(1, n_x):
            cross_copy(j, dx).wait_send()

    @pl.when(has_right)
    def _():
        halo_copy(0).wait_send()

    @pl.when(has_left)
    def _():
        halo_copy(1).wait_send()

    def drain(source, carry):
        for g in range(kvh):
            @pl.when(has_right & (source <= me))
            def _():
                block_copy(source, g, 0).wait_send()

            @pl.when(has_left & (source >= me))
            def _():
                block_copy(source, g, 1).wait_send()

        return carry

    lax.fori_loop(0, n, drain, 0)


def solution(mesh):
    n, n_tp = mesh.shape["sp"], mesh.shape["tp"]

    def per_device(wq, wk, wv, gq, gk, gv, sink, qgain, kgain, ww, gw):
        rows = wq.shape[0]
        kvh = wk.shape[1] // HEAD
        group = wq.shape[1] // wk.shape[1]
        model = ww.shape[1]
        chunks = 8
        width = model // chunks
        n_x = n_tp // 2
        out_rows = rows // n_tp
        heads_width = kvh * group * HEAD
        span = group * rows
        any_spec = pl.BlockSpec(memory_space=pl.ANY)
        vmem = pl.BlockSpec(memory_space=pltpu.VMEM)
        smem = pl.BlockSpec(memory_space=pltpu.SMEM)
        cross = max(n_x - 1, 1)
        return pl.pallas_call(
            functools.partial(kernel, n, n_tp, rows, kvh, group, chunks),
            out_shape=jax.ShapeDtypeStruct((out_rows, model), BF16),
            in_specs=[any_spec] * 6 + [smem, vmem, vmem, any_spec, any_spec],
            out_specs=vmem,
            scratch_shapes=[
                pltpu.VMEM((kvh, span, HEAD), BF16),
                pltpu.VMEM((kvh, 2, rows + 2 * WINDOW, HEAD), BF16),
                pltpu.VMEM((kvh, span, HEAD), BF16),
                pltpu.VMEM((kvh, rows, HEAD), BF16),
                pltpu.VMEM((kvh, span, HEAD), BF16),
                pltpu.VMEM((n, kvh, 2, rows, HEAD), BF16),
                pltpu.VMEM(ww.shape, BF16),
                pltpu.VMEM(gw.shape, BF16),
                pltpu.VMEM((rows, HEAD), F32),
                pltpu.VMEM((rows, HEAD), F32),
                pltpu.VMEM((kvh, 1, span), F32),
                pltpu.VMEM((kvh, 1, span), F32),
                pltpu.VMEM((kvh, HEAD, span), F32),
                pltpu.VMEM((rows, 2 * heads_width), BF16),
                pltpu.VMEM((rows, model), F32),
                pltpu.VMEM((chunks, 2, n_x, out_rows, width), BF16),
                pltpu.VMEM((chunks, n_x, out_rows, width), BF16),
                pltpu.VMEM((chunks, cross, out_rows, width), BF16),
                pltpu.VMEM((chunks, cross, out_rows, width), BF16),
                pltpu.VMEM((chunks, out_rows, width), F32),
                pltpu.SemaphoreType.DMA((4 * kvh + 2 * kvh * group + 2,)),
                pltpu.SemaphoreType.DMA((2, n, kvh)),
                pltpu.SemaphoreType.DMA((n, kvh)),
                pltpu.SemaphoreType.DMA((2,)),
                pltpu.SemaphoreType.DMA((2,)),
                pltpu.SemaphoreType.DMA((chunks,)),
                pltpu.SemaphoreType.DMA((chunks,)),
                pltpu.SemaphoreType.DMA((chunks, cross)),
                pltpu.SemaphoreType.DMA((chunks, cross)),
            ],
            compiler_params=pltpu.CompilerParams(
                collective_id=0, has_side_effects=True, vmem_limit_bytes=60 * 1024 * 1024
            ),
            name="hybrid",
        )(wq, wk, wv, gq, gk, gv, sink, qgain.reshape(1, HEAD), kgain.reshape(1, HEAD), ww, gw)

    return jax.shard_map(
        per_device,
        mesh=mesh,
        in_specs=(P(("grp", "sp"), "tp"),) * 6 + (P("tp"), P(), P(), P("tp", None), P("tp", None)),
        out_specs=P(("grp", "sp", "tp"), None),
        check_vma=False,
    )
```

```python
import functools
import math

import jax
import jax.numpy as jnp
from jax import lax
from jax.experimental import pallas as pl
from jax.experimental.pallas import tpu as pltpu
from jax.sharding import PartitionSpec as P

HEAD = 128
QH_A = 16
WINDOW = 128
GRID_W = 64
THETA = 10000.0
NEGATIVE = -1e30
EPSILON = 1e-06
MESH = pl.DeviceIdType.MESH
F32 = jnp.float32
BF16 = jnp.bfloat16


def dot_nt(a, b):
    return lax.dot_general(a, b, (((1,), (1,)), ((), ())), preferred_element_type=F32)


def dot_tn(a, b):
    return lax.dot_general(a, b, (((0,), (0,)), ((), ())), preferred_element_type=F32)


def kernel(
    n, n_tp, rows, kvh, group, chunks,
    wq_hbm, wk_hbm, wv_hbm, gq_hbm, gk_hbm, gv_hbm, sink_ref, qgain_ref, kgain_ref, ww_hbm, gw_hbm,
    out_hbm,
    qw, wkv, qraw, kraw, qg, kvbuf, ww, gw, cosine, sine, top, total, acc, attn, proj, pbuf, dbuf, sbuf, rbuf, own, out_ref,
    lsem, gsend, grecv, hsend, hrecv, dsend, drecv, xsend, xrecv, osem,
):
    me = lax.axis_index("sp")
    t = lax.axis_index("tp")
    core = lax.rem(t, 2)
    x = t // 2
    n_x = n_tp // 2
    partner = x * 2 + 1 - core
    out_rows = rows // n_tp
    width = ww.shape[1] // chunks
    span = group * rows
    has_left = me > 0
    has_right = me < n - 1

    loads = []

    def load(src, dst):
        copy = pltpu.make_async_copy(src, dst, lsem.at[len(loads)])
        copy.start()
        loads.append(copy)
        return copy

    def head_cols(h):
        return slice(h * HEAD, (h + 1) * HEAD)

    k_loads = [load(gk_hbm.at[:, head_cols(g)], kraw.at[g]) for g in range(kvh)]
    v_loads = [load(gv_hbm.at[:, head_cols(g)], kvbuf.at[me, g, 1]) for g in range(kvh)]
    w_loads = []
    for g in range(kvh):
        w_loads.append(load(wk_hbm.at[:, head_cols(g)], wkv.at[g, 0, WINDOW : WINDOW + rows]))
        w_loads.append(load(wv_hbm.at[:, head_cols(g)], wkv.at[g, 1, WINDOW : WINDOW + rows]))
    q_loads = []
    for g in range(kvh):
        for u in range(group):
            q_loads.append(load(gq_hbm.at[:, head_cols(g * group + u)], qraw.at[g, u * rows : (u + 1) * rows]))
    wq_loads = []
    for g in range(kvh):
        for u in range(group):
            wq_loads.append(load(wq_hbm.at[:, head_cols(g * group + u)], qw.at[g, u * rows : (u + 1) * rows]))
    ww_load = load(ww_hbm, ww)
    gw_load = load(gw_hbm, gw)

    barrier = pltpu.get_barrier_semaphore()

    def greet(device):
        pl.semaphore_signal(barrier, inc=1, device_id=device, device_id_type=MESH)

    @pl.when(has_left)
    def _():
        greet({"sp": me - 1})

    @pl.when(has_right)
    def _():
        greet({"sp": me + 1})

    greet({"tp": partner})
    for dx in range(1, n_x):
        greet({"tp": lax.rem(x + dx, n_x) * 2 + core})

    for copy in v_loads:
        copy.wait()

    pl.semaphore_wait(barrier, has_left.astype(jnp.int32) + has_right.astype(jnp.int32) + n_x)

    def block_copy(source, g, kind, direction):
        return pltpu.make_async_remote_copy(
            src_ref=kvbuf.at[source, g, kind],
            dst_ref=kvbuf.at[source, g, kind],
            send_sem=gsend.at[direction, source, g, kind],
            recv_sem=grecv.at[source, g, kind],
            device_id={"sp": me + 1 if direction == 0 else me - 1},
            device_id_type=MESH,
        )

    def halo_copy(direction):
        source = rows if direction == 0 else WINDOW
        target = 0 if direction == 0 else WINDOW + rows
        return pltpu.make_async_remote_copy(
            src_ref=wkv.at[:, :, source : source + WINDOW],
            dst_ref=wkv.at[:, :, target : target + WINDOW],
            send_sem=hsend.at[direction],
            recv_sem=hrecv.at[direction],
            device_id={"sp": me + 1 if direction == 0 else me - 1},
            device_id_type=MESH,
        )

    def send_own(g, kind):
        @pl.when(has_right)
        def _():
            block_copy(me, g, kind, 0).start()

        @pl.when(has_left)
        def _():
            block_copy(me, g, kind, 1).start()

    for g in range(kvh):
        send_own(g, 1)

    place = me * rows + lax.broadcasted_iota(jnp.int32, (rows, HEAD), 0)
    lane = lax.broadcasted_iota(jnp.int32, (rows, HEAD), 1)
    section = HEAD // 2
    half = section // 2
    frequency = jnp.exp(jnp.bitwise_and(lane, half - 1).astype(F32) * (-2.0 * math.log(THETA) / section))
    position = jnp.where(lane < section, place // GRID_W, lax.rem(place, GRID_W)).astype(F32)
    angle = position * frequency
    low = jnp.bitwise_and(lane, section - 1) < half
    cosine[...] = jnp.cos(angle)
    sine[...] = jnp.where(low, -jnp.sin(angle), jnp.sin(angle))

    def turn(values, gain):
        v = values.astype(F32)
        v = v * lax.rsqrt(jnp.mean(v * v, axis=1, keepdims=True) + EPSILON) * gain
        first = lax.broadcasted_iota(jnp.int32, v.shape, 1)
        other = jnp.where(
            jnp.bitwise_and(first, section - 1) < half,
            pltpu.roll(v, HEAD - half, 1),
            pltpu.roll(v, half, 1),
        )
        return (v * cosine[...] + other * sine[...]).astype(BF16)

    for g in range(kvh):
        k_loads[g].wait()
        kvbuf[me, g, 0] = turn(kraw[g], kgain_ref[...])
        send_own(g, 0)

    for copy in w_loads:
        copy.wait()

    @pl.when(has_right)
    def _():
        halo_copy(0).start()

    @pl.when(has_left)
    def _():
        halo_copy(1).start()

    @pl.when(jnp.logical_not(has_left))
    def _():
        wkv[:, :, 0:WINDOW] = jnp.zeros((kvh, 2, WINDOW, HEAD), BF16)

    @pl.when(jnp.logical_not(has_right))
    def _():
        wkv[:, :, WINDOW + rows :] = jnp.zeros((kvh, 2, WINDOW, HEAD), BF16)

    for copy in q_loads:
        copy.wait()
    for g in range(kvh):
        for u in range(group):
            part = slice(u * rows, (u + 1) * rows)
            qg[g, part] = turn(qraw[g, part], qgain_ref[...])

    scale = HEAD ** (-0.5)

    def absorb(source, g, first=False):
        scores = dot_nt(kvbuf[source, g, 0], qg[g]) * scale
        block_top = jnp.max(scores, axis=0, keepdims=True)
        if first:
            raised = jnp.exp(scores - block_top)
            top[g] = block_top
            total[g] = jnp.sum(raised, axis=0, keepdims=True)
            acc[g] = dot_tn(kvbuf[source, g, 1], raised.astype(BF16))
        else:
            before = top[g]
            new_top = jnp.maximum(before, block_top)
            fading = jnp.exp(before - new_top)
            raised = jnp.exp(scores - new_top)
            top[g] = new_top
            total[g] = total[g] * fading + jnp.sum(raised, axis=0, keepdims=True)
            acc[g] = acc[g] * fading + dot_tn(kvbuf[source, g, 1], raised.astype(BF16))

    for g in range(kvh):
        absorb(me, g, True)

    def hand_on(d, g, kind):
        @pl.when(me - d >= 0)
        def _():
            block_copy(me - d, g, kind, 0).wait_recv()

            @pl.when(has_right)
            def _():
                block_copy(me - d, g, kind, 0).start()

        @pl.when(me + d < n)
        def _():
            block_copy(me + d, g, kind, 1).wait_recv()

            @pl.when(has_left)
            def _():
                block_copy(me + d, g, kind, 1).start()

    def relay(d):
        for g in range(kvh):
            hand_on(d, g, 1)
        for g in range(kvh):
            hand_on(d, g, 0)

            @pl.when(me - d >= 0)
            def _():
                absorb(me - d, g)

            @pl.when(me + d < n)
            def _():
                absorb(me + d, g)

    def put_heads(base, g, value):
        turned = jnp.transpose(value).astype(BF16)
        for u in range(group):
            attn[:, base + (g * group + u) * HEAD : base + (g * group + u + 1) * HEAD] = turned[u * rows : (u + 1) * rows]

    heads_width = kvh * group * HEAD

    def windowed():
        for copy in wq_loads:
            copy.wait()

        @pl.when(has_left)
        def _():
            halo_copy(0).wait_recv()

        @pl.when(has_right)
        def _():
            halo_copy(1).wait_recv()

        padded = rows + 2 * WINDOW
        key_at = lax.broadcasted_iota(jnp.int32, (padded, span), 0) - WINDOW
        column = lax.broadcasted_iota(jnp.int32, (padded, span), 1)
        distance = jnp.abs(key_at - lax.rem(column, rows))
        key_place = me * rows + key_at
        inside = (distance <= WINDOW) & (key_place >= 0) & (key_place < n * rows)
        far = distance.astype(F32)
        member = lax.broadcasted_iota(jnp.int32, (1, span), 1) // rows
        for g in range(kvh):
            head = (t * (kvh * group) + g * group + 1 + member).astype(F32)
            slope = jnp.exp2(head * (-8.0 / QH_A))
            sink = jnp.zeros((1, span), F32)
            for u in range(group):
                sink = jnp.where(member == u, sink_ref[g * group + u], sink)
            scores = dot_nt(wkv[g, 0], qw[g]) * scale
            scores = jnp.where(inside, scores - slope * far, NEGATIVE)
            highest = jnp.maximum(jnp.max(scores, axis=0, keepdims=True), sink)
            raised = jnp.exp(scores - highest)
            bottom = jnp.sum(raised, axis=0, keepdims=True) + jnp.exp(sink - highest)
            weights = (raised * (1.0 / bottom)).astype(BF16)
            put_heads(0, g, dot_tn(wkv[g, 1], weights))
        ww_load.wait()
        for j in range(chunks):
            cols = slice(j * width, (j + 1) * width)
            proj[:, cols] = jnp.dot(attn[:, :heads_width], ww[:, cols], preferred_element_type=F32)

    if n > 1:
        relay(1)
    windowed()
    if n <= 4:
        for d in range(2, n):
            relay(d)
    else:
        def relay_step(d, carry):
            relay(d)
            return carry

        lax.fori_loop(2, n, relay_step, 0)

    for g in range(kvh):
        put_heads(heads_width, g, acc[g] * (1.0 / total[g]))
    gw_load.wait()

    def pair_copy(j):
        return pltpu.make_async_remote_copy(
            src_ref=pbuf.at[j, 1 - core],
            dst_ref=dbuf.at[j],
            send_sem=dsend.at[j],
            recv_sem=drecv.at[j],
            device_id={"tp": partner},
            device_id_type=MESH,
        )

    def cross_copy(j, dx):
        return pltpu.make_async_remote_copy(
            src_ref=sbuf.at[j, dx - 1],
            dst_ref=rbuf.at[j, dx - 1],
            send_sem=xsend.at[j, dx - 1],
            recv_sem=xrecv.at[j, dx - 1],
            device_id={"tp": lax.rem(x + dx, n_x) * 2 + core},
            device_id_type=MESH,
        )

    def pass_on(j):
        pair_copy(j).wait_recv()
        for dx in range(1, n_x):
            other = lax.rem(x + dx, n_x)
            sbuf[j, dx - 1] = (pbuf[j, core, other].astype(F32) + dbuf[j, other].astype(F32)).astype(BF16)
            cross_copy(j, dx).start()
        own[j] = pbuf[j, core, x].astype(F32) + dbuf[j, x].astype(F32)

    for j in range(chunks):
        cols = slice(j * width, (j + 1) * width)
        part = proj[:, cols] + jnp.dot(attn[:, heads_width:], gw[:, cols], preferred_element_type=F32)
        for b in range(n_tp):
            pbuf[j, b % 2, b // 2] = part[b * out_rows : (b + 1) * out_rows].astype(BF16)
        pair_copy(j).start()
        if j >= 1:
            pass_on(j - 1)
    pass_on(chunks - 1)

    def out_copy(j):
        cols = slice(j * width, (j + 1) * width)
        return pltpu.make_async_copy(out_ref.at[:, cols], out_hbm.at[:, cols], osem.at[j])

    for j in range(chunks):
        value = own[j]
        for dx in range(1, n_x):
            cross_copy(j, dx).wait_recv()
            value = value + rbuf[j, dx - 1].astype(F32)
        out_ref[:, j * width : (j + 1) * width] = value.astype(BF16)
        out_copy(j).start()

    for j in range(chunks):
        out_copy(j).wait()
        pair_copy(j).wait_send()
        for dx in range(1, n_x):
            cross_copy(j, dx).wait_send()

    @pl.when(has_right)
    def _():
        halo_copy(0).wait_send()

    @pl.when(has_left)
    def _():
        halo_copy(1).wait_send()

    def drain(source, carry):
        for g in range(kvh):
            for kind in range(2):
                @pl.when(has_right & (source <= me))
                def _():
                    block_copy(source, g, kind, 0).wait_send()

                @pl.when(has_left & (source >= me))
                def _():
                    block_copy(source, g, kind, 1).wait_send()

        return carry

    lax.fori_loop(0, n, drain, 0)


def solution(mesh):
    n, n_tp = mesh.shape["sp"], mesh.shape["tp"]

    def per_device(wq, wk, wv, gq, gk, gv, sink, qgain, kgain, ww, gw):
        rows = wq.shape[0]
        kvh = wk.shape[1] // HEAD
        group = wq.shape[1] // wk.shape[1]
        model = ww.shape[1]
        chunks = 8
        width = model // chunks
        n_x = n_tp // 2
        out_rows = rows // n_tp
        heads_width = kvh * group * HEAD
        span = group * rows
        any_spec = pl.BlockSpec(memory_space=pl.ANY)
        vmem = pl.BlockSpec(memory_space=pltpu.VMEM)
        smem = pl.BlockSpec(memory_space=pltpu.SMEM)
        cross = max(n_x - 1, 1)
        return pl.pallas_call(
            functools.partial(kernel, n, n_tp, rows, kvh, group, chunks),
            out_shape=jax.ShapeDtypeStruct((out_rows, model), BF16),
            in_specs=[any_spec] * 6 + [smem, vmem, vmem, any_spec, any_spec],
            out_specs=any_spec,
            scratch_shapes=[
                pltpu.VMEM((kvh, span, HEAD), BF16),
                pltpu.VMEM((kvh, 2, rows + 2 * WINDOW, HEAD), BF16),
                pltpu.VMEM((kvh, span, HEAD), BF16),
                pltpu.VMEM((kvh, rows, HEAD), BF16),
                pltpu.VMEM((kvh, span, HEAD), BF16),
                pltpu.VMEM((n, kvh, 2, rows, HEAD), BF16),
                pltpu.VMEM(ww.shape, BF16),
                pltpu.VMEM(gw.shape, BF16),
                pltpu.VMEM((rows, HEAD), F32),
                pltpu.VMEM((rows, HEAD), F32),
                pltpu.VMEM((kvh, 1, span), F32),
                pltpu.VMEM((kvh, 1, span), F32),
                pltpu.VMEM((kvh, HEAD, span), F32),
                pltpu.VMEM((rows, 2 * heads_width), BF16),
                pltpu.VMEM((rows, model), F32),
                pltpu.VMEM((chunks, 2, n_x, out_rows, width), BF16),
                pltpu.VMEM((chunks, n_x, out_rows, width), BF16),
                pltpu.VMEM((chunks, cross, out_rows, width), BF16),
                pltpu.VMEM((chunks, cross, out_rows, width), BF16),
                pltpu.VMEM((chunks, out_rows, width), F32),
                pltpu.VMEM((out_rows, model), BF16),
                pltpu.SemaphoreType.DMA((4 * kvh + 2 * kvh * group + 2,)),
                pltpu.SemaphoreType.DMA((2, n, kvh, 2)),
                pltpu.SemaphoreType.DMA((n, kvh, 2)),
                pltpu.SemaphoreType.DMA((2,)),
                pltpu.SemaphoreType.DMA((2,)),
                pltpu.SemaphoreType.DMA((chunks,)),
                pltpu.SemaphoreType.DMA((chunks,)),
                pltpu.SemaphoreType.DMA((chunks, cross)),
                pltpu.SemaphoreType.DMA((chunks, cross)),
                pltpu.SemaphoreType.DMA((chunks,)),
            ],
            compiler_params=pltpu.CompilerParams(
                collective_id=0, has_side_effects=True, vmem_limit_bytes=60 * 1024 * 1024
            ),
            name="hybrid",
        )(wq, wk, wv, gq, gk, gv, sink, qgain.reshape(1, HEAD), kgain.reshape(1, HEAD), ww, gw)

    return jax.shard_map(
        per_device,
        mesh=mesh,
        in_specs=(P(("grp", "sp"), "tp"),) * 6 + (P("tp"), P(), P(), P("tp", None), P("tp", None)),
        out_specs=P(("grp", "sp", "tp"), None),
        check_vma=False,
    )
```

```python
import functools
import math

import jax
import jax.numpy as jnp
from jax import lax
from jax.experimental import pallas as pl
from jax.experimental.pallas import tpu as pltpu
from jax.sharding import PartitionSpec as P

HEAD = 128
QH_A = 16
WINDOW = 128
GRID_W = 64
THETA = 10000.0
NEGATIVE = -1e30
EPSILON = 1e-06
MESH = pl.DeviceIdType.MESH
F32 = jnp.float32
BF16 = jnp.bfloat16


def dot_nt(a, b):
    return lax.dot_general(a, b, (((1,), (1,)), ((), ())), preferred_element_type=F32)


def dot_tn(a, b):
    return lax.dot_general(a, b, (((0,), (0,)), ((), ())), preferred_element_type=F32)


def kernel(
    n, n_tp, rows, kvh, group, chunks,
    wq_hbm, wk_hbm, wv_hbm, gq_hbm, gk_hbm, gv_hbm, sink_ref, qgain_ref, kgain_ref, ww_hbm, gw_hbm,
    out_hbm,
    qw, wkv, qraw, kraw, qg, kvbuf, ww, gw, cosine, sine, top, total, acc, attn, proj, pbuf, dbuf, sbuf, rbuf, own, out_ref,
    lsem, gsend, grecv, hsend, hrecv, dsend, drecv, xsend, xrecv, osem,
):
    me = lax.axis_index("sp")
    t = lax.axis_index("tp")
    core = lax.rem(t, 2)
    x = t // 2
    n_x = n_tp // 2
    partner = x * 2 + 1 - core
    out_rows = rows // n_tp
    width = ww.shape[1] // chunks
    span = group * rows
    has_left = me > 0
    has_right = me < n - 1

    loads = []

    def load(src, dst):
        copy = pltpu.make_async_copy(src, dst, lsem.at[len(loads)])
        copy.start()
        loads.append(copy)
        return copy

    def head_cols(h):
        return slice(h * HEAD, (h + 1) * HEAD)

    k_loads = [load(gk_hbm.at[:, head_cols(g)], kraw.at[g]) for g in range(kvh)]
    v_loads = [load(gv_hbm.at[:, head_cols(g)], kvbuf.at[me, g, 1]) for g in range(kvh)]
    w_loads = []
    for g in range(kvh):
        w_loads.append(load(wk_hbm.at[:, head_cols(g)], wkv.at[g, 0, WINDOW : WINDOW + rows]))
        w_loads.append(load(wv_hbm.at[:, head_cols(g)], wkv.at[g, 1, WINDOW : WINDOW + rows]))
    q_loads = []
    for g in range(kvh):
        for u in range(group):
            q_loads.append(load(gq_hbm.at[:, head_cols(g * group + u)], qraw.at[g, u * rows : (u + 1) * rows]))
    wq_loads = []
    for g in range(kvh):
        for u in range(group):
            wq_loads.append(load(wq_hbm.at[:, head_cols(g * group + u)], qw.at[g, u * rows : (u + 1) * rows]))
    ww_load = load(ww_hbm, ww)
    gw_load = load(gw_hbm, gw)

    barrier = pltpu.get_barrier_semaphore()

    def greet(device):
        pl.semaphore_signal(barrier, inc=1, device_id=device, device_id_type=MESH)

    @pl.when(has_left)
    def _():
        greet({"sp": me - 1})

    @pl.when(has_right)
    def _():
        greet({"sp": me + 1})

    greet({"tp": partner})
    for dx in range(1, n_x):
        greet({"tp": lax.rem(x + dx, n_x) * 2 + core})

    for copy in v_loads:
        copy.wait()

    pl.semaphore_wait(barrier, has_left.astype(jnp.int32) + has_right.astype(jnp.int32) + n_x)

    def block_copy(source, g, kind, direction):
        return pltpu.make_async_remote_copy(
            src_ref=kvbuf.at[source, g, kind],
            dst_ref=kvbuf.at[source, g, kind],
            send_sem=gsend.at[direction, source, g, kind],
            recv_sem=grecv.at[source, g, kind],
            device_id={"sp": me + 1 if direction == 0 else me - 1},
            device_id_type=MESH,
        )

    def halo_copy(direction):
        source = rows if direction == 0 else WINDOW
        target = 0 if direction == 0 else WINDOW + rows
        return pltpu.make_async_remote_copy(
            src_ref=wkv.at[:, :, source : source + WINDOW],
            dst_ref=wkv.at[:, :, target : target + WINDOW],
            send_sem=hsend.at[direction],
            recv_sem=hrecv.at[direction],
            device_id={"sp": me + 1 if direction == 0 else me - 1},
            device_id_type=MESH,
        )

    def send_own(g, kind):
        @pl.when(has_right)
        def _():
            block_copy(me, g, kind, 0).start()

        @pl.when(has_left)
        def _():
            block_copy(me, g, kind, 1).start()

    for g in range(kvh):
        send_own(g, 1)

    place = me * rows + lax.broadcasted_iota(jnp.int32, (rows, HEAD), 0)
    lane = lax.broadcasted_iota(jnp.int32, (rows, HEAD), 1)
    section = HEAD // 2
    half = section // 2
    frequency = jnp.exp(jnp.bitwise_and(lane, half - 1).astype(F32) * (-2.0 * math.log(THETA) / section))
    position = jnp.where(lane < section, place // GRID_W, lax.rem(place, GRID_W)).astype(F32)
    angle = position * frequency
    low = jnp.bitwise_and(lane, section - 1) < half
    both = jnp.cos(jnp.where(low, angle, angle - 0.5 * math.pi))
    cosine[...] = jnp.where(low, both, pltpu.roll(both, half, 1))
    sine[...] = jnp.where(low, -pltpu.roll(both, HEAD - half, 1), both)

    def turn(values, gain):
        v = values.astype(F32)
        v = v * lax.rsqrt(jnp.mean(v * v, axis=1, keepdims=True) + EPSILON) * gain
        first = lax.broadcasted_iota(jnp.int32, v.shape, 1)
        other = jnp.where(
            jnp.bitwise_and(first, section - 1) < half,
            pltpu.roll(v, HEAD - half, 1),
            pltpu.roll(v, half, 1),
        )
        return (v * cosine[...] + other * sine[...]).astype(BF16)

    for g in range(kvh):
        k_loads[g].wait()
        kvbuf[me, g, 0] = turn(kraw[g], kgain_ref[...])
        send_own(g, 0)

    for copy in w_loads:
        copy.wait()

    @pl.when(has_right)
    def _():
        halo_copy(0).start()

    @pl.when(has_left)
    def _():
        halo_copy(1).start()

    @pl.when(jnp.logical_not(has_left))
    def _():
        wkv[:, :, 0:WINDOW] = jnp.zeros((kvh, 2, WINDOW, HEAD), BF16)

    @pl.when(jnp.logical_not(has_right))
    def _():
        wkv[:, :, WINDOW + rows :] = jnp.zeros((kvh, 2, WINDOW, HEAD), BF16)

    for copy in q_loads:
        copy.wait()
    for g in range(kvh):
        for u in range(group):
            part = slice(u * rows, (u + 1) * rows)
            qg[g, part] = turn(qraw[g, part], qgain_ref[...])

    scale = HEAD ** (-0.5)

    def absorb(source, g, first=False):
        scores = dot_nt(kvbuf[source, g, 0], qg[g]) * scale
        block_top = jnp.max(scores, axis=0, keepdims=True)
        if first:
            raised = jnp.exp(scores - block_top)
            top[g] = block_top
            total[g] = jnp.sum(raised, axis=0, keepdims=True)
            acc[g] = dot_tn(kvbuf[source, g, 1], raised.astype(BF16))
        else:
            before = top[g]
            new_top = jnp.maximum(before, block_top)
            fading = jnp.exp(before - new_top)
            raised = jnp.exp(scores - new_top)
            top[g] = new_top
            total[g] = total[g] * fading + jnp.sum(raised, axis=0, keepdims=True)
            acc[g] = acc[g] * fading + dot_tn(kvbuf[source, g, 1], raised.astype(BF16))

    for g in range(kvh):
        absorb(me, g, True)

    def hand_on(d, g, kind):
        @pl.when(me - d >= 0)
        def _():
            block_copy(me - d, g, kind, 0).wait_recv()

            @pl.when(has_right)
            def _():
                block_copy(me - d, g, kind, 0).start()

        @pl.when(me + d < n)
        def _():
            block_copy(me + d, g, kind, 1).wait_recv()

            @pl.when(has_left)
            def _():
                block_copy(me + d, g, kind, 1).start()

    def relay(d):
        for g in range(kvh):
            hand_on(d, g, 1)
        for g in range(kvh):
            hand_on(d, g, 0)

            @pl.when(me - d >= 0)
            def _():
                absorb(me - d, g)

            @pl.when(me + d < n)
            def _():
                absorb(me + d, g)

    def put_heads(base, g, value):
        turned = jnp.transpose(value).astype(BF16)
        for u in range(group):
            attn[:, base + (g * group + u) * HEAD : base + (g * group + u + 1) * HEAD] = turned[u * rows : (u + 1) * rows]

    heads_width = kvh * group * HEAD

    def windowed():
        for copy in wq_loads:
            copy.wait()

        @pl.when(has_left)
        def _():
            halo_copy(0).wait_recv()

        @pl.when(has_right)
        def _():
            halo_copy(1).wait_recv()

        padded = rows + 2 * WINDOW
        key_at = lax.broadcasted_iota(jnp.int32, (padded, span), 0) - WINDOW
        column = lax.broadcasted_iota(jnp.int32, (padded, span), 1)
        distance = jnp.abs(key_at - lax.rem(column, rows))
        key_place = me * rows + key_at
        inside = (distance <= WINDOW) & (key_place >= 0) & (key_place < n * rows)
        far = distance.astype(F32)
        member = lax.broadcasted_iota(jnp.int32, (1, span), 1) // rows
        for g in range(kvh):
            head = (t * (kvh * group) + g * group + 1 + member).astype(F32)
            slope = jnp.exp2(head * (-8.0 / QH_A))
            sink = jnp.zeros((1, span), F32)
            for u in range(group):
                sink = jnp.where(member == u, sink_ref[g * group + u], sink)
            scores = dot_nt(wkv[g, 0], qw[g]) * scale
            scores = jnp.where(inside, scores - slope * far, NEGATIVE)
            highest = jnp.maximum(jnp.max(scores, axis=0, keepdims=True), sink)
            raised = jnp.exp(scores - highest)
            bottom = jnp.sum(raised, axis=0, keepdims=True) + jnp.exp(sink - highest)
            weights = (raised * (1.0 / bottom)).astype(BF16)
            put_heads(0, g, dot_tn(wkv[g, 1], weights))
        ww_load.wait()
        for j in range(chunks):
            cols = slice(j * width, (j + 1) * width)
            proj[:, cols] = jnp.dot(attn[:, :heads_width], ww[:, cols], preferred_element_type=F32)

    if n > 1:
        relay(1)
    windowed()
    if n <= 4:
        for d in range(2, n):
            relay(d)
    else:
        def relay_step(d, carry):
            relay(d)
            return carry

        lax.fori_loop(2, n, relay_step, 0)

    for g in range(kvh):
        put_heads(heads_width, g, acc[g] * (1.0 / total[g]))
    gw_load.wait()

    def pair_copy(j):
        return pltpu.make_async_remote_copy(
            src_ref=pbuf.at[j, 1 - core],
            dst_ref=dbuf.at[j],
            send_sem=dsend.at[j],
            recv_sem=drecv.at[j],
            device_id={"tp": partner},
            device_id_type=MESH,
        )

    def cross_copy(j, dx):
        return pltpu.make_async_remote_copy(
            src_ref=sbuf.at[j, dx - 1],
            dst_ref=rbuf.at[j, dx - 1],
            send_sem=xsend.at[j, dx - 1],
            recv_sem=xrecv.at[j, dx - 1],
            device_id={"tp": lax.rem(x + dx, n_x) * 2 + core},
            device_id_type=MESH,
        )

    def pass_on(j):
        pair_copy(j).wait_recv()
        for dx in range(1, n_x):
            other = lax.rem(x + dx, n_x)
            sbuf[j, dx - 1] = (pbuf[j, core, other].astype(F32) + dbuf[j, other].astype(F32)).astype(BF16)
            cross_copy(j, dx).start()
        own[j] = pbuf[j, core, x].astype(F32) + dbuf[j, x].astype(F32)

    for j in range(chunks):
        cols = slice(j * width, (j + 1) * width)
        part = proj[:, cols] + jnp.dot(attn[:, heads_width:], gw[:, cols], preferred_element_type=F32)
        for b in range(n_tp):
            pbuf[j, b % 2, b // 2] = part[b * out_rows : (b + 1) * out_rows].astype(BF16)
        pair_copy(j).start()
        if j >= 1:
            pass_on(j - 1)
    pass_on(chunks - 1)

    def out_copy(j):
        cols = slice(j * width, (j + 1) * width)
        return pltpu.make_async_copy(out_ref.at[:, cols], out_hbm.at[:, cols], osem.at[j])

    for j in range(chunks):
        value = own[j]
        for dx in range(1, n_x):
            cross_copy(j, dx).wait_recv()
            value = value + rbuf[j, dx - 1].astype(F32)
        out_ref[:, j * width : (j + 1) * width] = value.astype(BF16)
        out_copy(j).start()

    for j in range(chunks):
        out_copy(j).wait()
        pair_copy(j).wait_send()
        for dx in range(1, n_x):
            cross_copy(j, dx).wait_send()

    @pl.when(has_right)
    def _():
        halo_copy(0).wait_send()

    @pl.when(has_left)
    def _():
        halo_copy(1).wait_send()

    def drain(source, carry):
        for g in range(kvh):
            for kind in range(2):
                @pl.when(has_right & (source <= me))
                def _():
                    block_copy(source, g, kind, 0).wait_send()

                @pl.when(has_left & (source >= me))
                def _():
                    block_copy(source, g, kind, 1).wait_send()

        return carry

    lax.fori_loop(0, n, drain, 0)


def solution(mesh):
    n, n_tp = mesh.shape["sp"], mesh.shape["tp"]

    def per_device(wq, wk, wv, gq, gk, gv, sink, qgain, kgain, ww, gw):
        rows = wq.shape[0]
        kvh = wk.shape[1] // HEAD
        group = wq.shape[1] // wk.shape[1]
        model = ww.shape[1]
        chunks = 8
        width = model // chunks
        n_x = n_tp // 2
        out_rows = rows // n_tp
        heads_width = kvh * group * HEAD
        span = group * rows
        any_spec = pl.BlockSpec(memory_space=pl.ANY)
        vmem = pl.BlockSpec(memory_space=pltpu.VMEM)
        smem = pl.BlockSpec(memory_space=pltpu.SMEM)
        cross = max(n_x - 1, 1)
        return pl.pallas_call(
            functools.partial(kernel, n, n_tp, rows, kvh, group, chunks),
            out_shape=jax.ShapeDtypeStruct((out_rows, model), BF16),
            in_specs=[any_spec] * 6 + [smem, vmem, vmem, any_spec, any_spec],
            out_specs=any_spec,
            scratch_shapes=[
                pltpu.VMEM((kvh, span, HEAD), BF16),
                pltpu.VMEM((kvh, 2, rows + 2 * WINDOW, HEAD), BF16),
                pltpu.VMEM((kvh, span, HEAD), BF16),
                pltpu.VMEM((kvh, rows, HEAD), BF16),
                pltpu.VMEM((kvh, span, HEAD), BF16),
                pltpu.VMEM((n, kvh, 2, rows, HEAD), BF16),
                pltpu.VMEM(ww.shape, BF16),
                pltpu.VMEM(gw.shape, BF16),
                pltpu.VMEM((rows, HEAD), F32),
                pltpu.VMEM((rows, HEAD), F32),
                pltpu.VMEM((kvh, 1, span), F32),
                pltpu.VMEM((kvh, 1, span), F32),
                pltpu.VMEM((kvh, HEAD, span), F32),
                pltpu.VMEM((rows, 2 * heads_width), BF16),
                pltpu.VMEM((rows, model), F32),
                pltpu.VMEM((chunks, 2, n_x, out_rows, width), BF16),
                pltpu.VMEM((chunks, n_x, out_rows, width), BF16),
                pltpu.VMEM((chunks, cross, out_rows, width), BF16),
                pltpu.VMEM((chunks, cross, out_rows, width), BF16),
                pltpu.VMEM((chunks, out_rows, width), F32),
                pltpu.VMEM((out_rows, model), BF16),
                pltpu.SemaphoreType.DMA((4 * kvh + 2 * kvh * group + 2,)),
                pltpu.SemaphoreType.DMA((2, n, kvh, 2)),
                pltpu.SemaphoreType.DMA((n, kvh, 2)),
                pltpu.SemaphoreType.DMA((2,)),
                pltpu.SemaphoreType.DMA((2,)),
                pltpu.SemaphoreType.DMA((chunks,)),
                pltpu.SemaphoreType.DMA((chunks,)),
                pltpu.SemaphoreType.DMA((chunks, cross)),
                pltpu.SemaphoreType.DMA((chunks, cross)),
                pltpu.SemaphoreType.DMA((chunks,)),
            ],
            compiler_params=pltpu.CompilerParams(
                collective_id=0, has_side_effects=True, vmem_limit_bytes=60 * 1024 * 1024
            ),
            name="hybrid",
        )(wq, wk, wv, gq, gk, gv, sink, qgain.reshape(1, HEAD), kgain.reshape(1, HEAD), ww, gw)

    return jax.shard_map(
        per_device,
        mesh=mesh,
        in_specs=(P(("grp", "sp"), "tp"),) * 6 + (P("tp"), P(), P(), P("tp", None), P("tp", None)),
        out_specs=P(("grp", "sp", "tp"), None),
        check_vma=False,
    )
```
